32 devices in a mesh: ep: 8 (over z, x), tp: 4 (over y, core).
Axes of the slice: x: 2, y: 2, z: 4, core: 2. Of those that a mesh axis runs over, the one named last changes fastest.
Arguments:
- tokens: bfloat16 [1024, 1024], P('ep', 'tp'), may hold values from -6 to 6
- cotangent: bfloat16 [1024, 1024], P('ep', 'tp'), may hold values from -4 to 4
- routes: int32 [1024, 2], P('ep'), may hold values from 0 to 7, all different within a row; in each aligned block of 128 rows (0 to 127, 128 to 255, ...) at most 40 rows name the same one
- route_weights: bfloat16 [1024, 2], P('ep'), may hold values from 0.099609375 to 0.8984375
- w_gate: bfloat16 [8, 1024, 2816], P('ep', None, 'tp'), may hold values from -0.1875 to 0.1875
- w_up: bfloat16 [8, 1024, 2816], P('ep', None, 'tp'), may hold values from -0.1875 to 0.1875
- w_down: bfloat16 [8, 2816, 1024], P('ep', 'tp'), may hold values from -0.109375 to 0.109375
- dense_weight: bfloat16 [1024, 1024], P('tp', 'ep'), may hold values from -0.25 to 0.25
- mix_gate: float32 [1024], replicated, may hold values from 0.1 to 1.9
Outputs:
- token_grad: bfloat16 [1024, 1024], P('ep', 'tp')
- route_grad: float32 [1024, 2], P('ep')
- gate_grad: bfloat16 [8, 1024, 2816], P('ep', None, 'tp')
- up_grad: bfloat16 [8, 1024, 2816], P('ep', None, 'tp')
- down_grad: bfloat16 [8, 2816, 1024], P('ep', 'tp')
- dense_grad: float32 [1024, 1024], P('tp', 'ep')
- mix_grad: float32 [1024], replicated
The draws below stay inside these ranges and needn't reach their ends.
Inputs may be any that keep to these rules, and one draw needn't show every extreme that they name: `routes`: each row names 2 different experts. In the rows of one index of ep (aligned blocks of 128 rows) no expert is named by more than 40 rows, a bound that some block reaches.
All inputs are finite; a program needn't handle non-finite values.
Results may differ from the reference program's by a relative error of at most 0.0065.
Values may be sent and summed in bfloat16 or wider, within the bound.
A program may use at most 64 MiB of HBM per device.

```python
import math
import jax
import jax.numpy as jnp
import numpy as np
from jax import lax

D = 1024
FF = 2816
TOP = 2
TOK_DEV = 128
GROUP = 1
EXPERTS = 8
CAP = 40
FFB = 2816
SLICE = 704
TOKENS = 1024
N_EP = 8
N_TP = 4


def strengthened(values, stream_key, source, target, shards_of, factor):
    owner, partner = [(jnp.arange(values.shape[axis_at]) // (values.shape[axis_at] // shards_of)).reshape([-1 if axis == axis_at else 1 for axis in range(values.ndim)]) for axis_at in (source, target)]
    chosen = jax.random.permutation(stream_key, shards_of)[partner]
    strong = (owner == chosen) | (owner == (partner + shards_of // 2) % shards_of)
    return jnp.where(strong, factor * values, values)


def block_scale(stream_key, dims, pieces, smallest, top_value):
    factor_of, own = 1.0, jax.random.fold_in(stream_key, 6)
    for dim, blocks in pieces:
        draws = jnp.exp(jax.random.uniform(jax.random.fold_in(own, dim), (blocks,), jnp.float32, smallest / len(pieces), top_value / len(pieces)))
        factor_of = factor_of * jnp.repeat(draws, dims[dim] // blocks).reshape([-1 if axis == dim else 1 for axis in range(len(dims))])
    return factor_of


def deal_out(own_key, own, number, rows, number_of, top, limit, lean):
    sequence = jax.random.permutation(own_key, number_of)
    packed, ordinary = shares(number_of, rows * top, limit, lean, True), shares(number_of, rows * top, limit, lean, False)
    places = jnp.arange(number_of)

    def named(sizes, offset_by):
        used = int((sizes > 0).sum())
        fixed = max(1, used // 4)
        passed = fixed + (places - fixed + offset_by * (used - fixed)) % max(1, number_of - fixed)
        return jnp.zeros((number_of,), jnp.int32).at[sequence[jnp.where(places < fixed, places, passed)]].set(jnp.asarray(sizes, jnp.int32))

    sizes = jnp.where(number % 4 == 0, named(packed, number // 4), named(ordinary, number - number // 4 - 1))
    mixed = jax.random.permutation(jax.random.fold_in(own, 3), number_of)
    donor, taker = mixed[0:number_of // 2 * 2:2], mixed[1:number_of // 2 * 2:2]
    room = jnp.minimum(sizes[donor] - 1, limit - sizes[taker]) // 2
    room = jnp.where((donor == sequence[0]) | (taker == sequence[0]) | (sizes[taker] == 0), 0, jnp.maximum(room, 0))
    passed = jax.random.randint(jax.random.fold_in(own, 4), (number_of // 2,), 0, 1 << 20) % (room + 1)
    sizes = sizes.at[donor].add(-passed).at[taker].add(passed)
    labels = jnp.searchsorted(jnp.cumsum(sizes), jnp.arange(rows * top), side="right").astype(jnp.int32)
    listing = labels.reshape(top, rows).T
    listing = listing[jax.random.permutation(jax.random.fold_in(own, 1), rows)]
    offset_by = jax.random.randint(jax.random.fold_in(own, 2), (rows, 1), 0, top)
    return jnp.take_along_axis(listing, (jnp.arange(top)[None, :] + offset_by) % top, axis=1)


def shares(amount, total, limit, lean, full):
    loads = [(1 << 20) // math.isqrt(rank ** lean) + 1 for rank in range(1, amount + 1)]
    largest = limit if full else min(limit, max(-(-total // amount), total * loads[0] // sum(loads)))
    least = 1 if total - largest >= amount - 1 else 0
    counts, surplus = [largest] + [least] * (amount - 1), total - largest - least * (amount - 1)
    while surplus > 0:
        movable = [i for i in range(1, amount) if counts[i] < largest] or [i for i in range(1, amount) if counts[i] < limit]
        mass, left = sum([loads[i] for i in movable]), surplus
        for i in movable:
            extra = min(limit - counts[i], max(1, left * loads[i] // mass), surplus)
            counts[i] = counts[i] + extra
            surplus = surplus - extra
    return np.array(counts)


def noise(key, dims, scale, most, shards=(), held_as=jnp.bfloat16):
    drawn = scale * jax.random.normal(key, dims, jnp.float32)
    if shards:
        drawn = drawn * block_scale(key, dims, shards, -0.22, 0.18)
    return jnp.clip(drawn, -most, most).astype(held_as)


def noise_with(own_key, extent, width, most, cuts, heavy, kind=jnp.bfloat16):
    values = width * jax.random.normal(own_key, extent, jnp.float32)
    if cuts:
        values = values * block_scale(own_key, extent, cuts, -0.22, 0.18)
    return jnp.clip(strengthened(values, jax.random.fold_in(own_key, 3), *heavy), -most, most).astype(kind)


def setup_inputs(seed: int = 0) -> dict:
    streams_of = jax.random.split(jax.random.key(seed), 10)
    tokens = noise(streams_of[0], (TOKENS, D), 1.0, 6.0, ((0, 8), (1, 4)))
    cotangent = noise_with(streams_of[1], (TOKENS, D), 0.5, 4.0, ((0, 8), (1, 4)), (0, 1, 8, 2.0))
    routes_keys = jax.random.split(jax.random.fold_in(streams_of[2], 1), TOKENS // TOK_DEV)
    routes_turns = jax.random.permutation(jax.random.fold_in(streams_of[2], 3), TOKENS // TOK_DEV)
    routes = jax.vmap(lambda own, number: deal_out(jax.random.fold_in(streams_of[2], 2), own, number, TOK_DEV, EXPERTS, TOP, CAP, 2))(routes_keys, routes_turns).reshape((TOKENS, TOP))
    route_weights = jnp.clip(0.099609375 + 0.7988281 * jax.random.uniform(streams_of[3], (TOKENS, TOP), jnp.float32) ** block_scale(streams_of[3], (TOKENS, TOP), ((0, 8),), -0.2, 0.2), 0.099609375, 0.8984375).astype(jnp.bfloat16)
    w_gate = noise(streams_of[4], (EXPERTS * GROUP, D, FFB), D ** -0.5, 0.1875, ((0, 8), (2, 4)))
    w_up = noise(streams_of[5], (EXPERTS * GROUP, D, FFB), D ** -0.5, 0.1875, ((0, 8), (2, 4)))
    w_down = noise(streams_of[6], (EXPERTS * GROUP, FFB, D), FF ** -0.5, 0.109375, ((0, 8), (1, 4)))
    dense_weight = noise_with(streams_of[7], (D, D), D ** -0.5, 0.25, ((0, 4), (1, 8)), (1, 0, 8, 2.0))
    mix_gate = jnp.clip(1.0 + 0.18 * jax.random.normal(streams_of[8], (D,), jnp.float32), 0.1, 1.9)
    return dict(tokens=tokens, cotangent=cotangent, routes=routes, route_weights=route_weights, w_gate=w_gate, w_up=w_up, w_down=w_down, dense_weight=dense_weight, mix_gate=mix_gate)


def reference(tokens, cotangent, routes, route_weights, w_gate, w_up, w_down, dense_weight, mix_gate):
    picks = TOK_DEV * TOP
    slots = EXPERTS * CAP
    blocked = routes.reshape(N_EP, picks)
    onehot = (blocked[:, :, None] == jnp.arange(EXPERTS, dtype=jnp.int32)[None, None, :]).astype(jnp.int32)
    ranking = jnp.cumsum(onehot, axis=1) - 1
    target = (blocked * CAP + jnp.sum(onehot * ranking, axis=2)).astype(jnp.int32)
    pick_index = jnp.arange(picks, dtype=jnp.int32)
    block_base = (jnp.arange(N_EP, dtype=jnp.int32) * TOK_DEV)[:, None]
    token_index = (block_base + pick_index[None, :] // TOP).astype(jnp.int32)
    block_rows = jnp.broadcast_to(jnp.arange(N_EP, dtype=jnp.int32)[:, None], target.shape)
    source = jnp.zeros((N_EP, slots), jnp.int32).at[block_rows, target].set(token_index)
    pick_slot = jnp.zeros((N_EP, slots), jnp.int32).at[block_rows, target].set(
        jnp.broadcast_to(pick_index[None, :] % TOP, target.shape).astype(jnp.int32))
    filled = jnp.zeros((N_EP, slots), jnp.float32).at[block_rows, target].set(1.0)
    slot_weight = jnp.zeros((N_EP, slots), jnp.float32).at[block_rows, target].set(
        route_weights.reshape(N_EP, picks).astype(jnp.float32))

    def by_expert(table):
        return table.reshape(N_EP, EXPERTS, CAP).transpose(1, 0, 2).reshape(EXPERTS, N_EP * CAP)

    gate_blocks = w_gate.reshape(EXPERTS, GROUP, D, FFB)
    up_blocks = w_up.reshape(EXPERTS, GROUP, D, FFB)
    down_blocks = w_down.reshape(EXPERTS, GROUP, FFB, D)
    slices = GROUP * N_TP

    def one_expert(carry, inputs):
        token_acc, route_acc = carry
        src, kslot, live, weight, gate_b, up_b, down_b = inputs
        token_rows = tokens[src]
        grad_rows = cotangent[src]
        gate_matrix = gate_b.transpose(1, 0, 2).reshape(D, FF)
        up_matrix = up_b.transpose(1, 0, 2).reshape(D, FF)
        down_matrix = down_b.reshape(FF, D)
        pre_gate = jnp.dot(token_rows, gate_matrix, preferred_element_type=jnp.float32)
        pre_up = jnp.dot(token_rows, up_matrix, preferred_element_type=jnp.float32)
        sigmoid_gate = jax.nn.sigmoid(pre_gate)
        activated = pre_gate * sigmoid_gate
        hidden = activated * pre_up
        hidden_bf = hidden.astype(jnp.bfloat16)
        projected = jnp.dot(grad_rows, down_matrix.T, preferred_element_type=jnp.float32)
        route_part = jnp.sum(hidden_bf.astype(jnp.float32) * projected, axis=1)
        weight_col = weight[:, None]
        hidden_grad = weight_col * projected
        d_gate = (hidden_grad * pre_up * sigmoid_gate * (1.0 + pre_gate * (1.0 - sigmoid_gate))).astype(jnp.bfloat16)
        d_up = (hidden_grad * activated).astype(jnp.bfloat16)
        weighted = (weight_col * hidden).astype(jnp.bfloat16)
        gate_delta = jnp.dot(token_rows.T, d_gate, preferred_element_type=jnp.float32).astype(jnp.bfloat16)
        up_delta = jnp.dot(token_rows.T, d_up, preferred_element_type=jnp.float32).astype(jnp.bfloat16)
        down_delta = jnp.dot(weighted.T, grad_rows, preferred_element_type=jnp.float32).astype(jnp.bfloat16)
        row_count = token_rows.shape[0]
        gate_slices = d_gate.astype(jnp.float32).reshape(row_count, slices, SLICE)
        up_slices = d_up.astype(jnp.float32).reshape(row_count, slices, SLICE)
        gate_cols = gate_matrix.astype(jnp.float32).reshape(D, slices, SLICE)
        up_cols = up_matrix.astype(jnp.float32).reshape(D, slices, SLICE)
        partial_value = (jnp.einsum('rsf,dsf->rsd', gate_slices, gate_cols)
                   + jnp.einsum('rsf,dsf->rsd', up_slices, up_cols)).astype(jnp.bfloat16)
        block_sum = jnp.sum(partial_value.reshape(row_count, GROUP, N_TP, D).astype(jnp.float32), axis=2).astype(jnp.bfloat16)
        summed = jnp.sum(block_sum.astype(jnp.float32), axis=1)
        token_acc = token_acc.at[src].add(summed * live[:, None])
        route_acc = route_acc.at[src, kslot].add(route_part * live)
        outputs = (gate_delta.reshape(D, GROUP, FFB).transpose(1, 0, 2),
                   up_delta.reshape(D, GROUP, FFB).transpose(1, 0, 2),
                   down_delta.reshape(GROUP, FFB, D))
        return (token_acc, route_acc), outputs

    start = (jnp.zeros((TOKENS, D), jnp.float32), jnp.zeros((TOKENS, TOP), jnp.float32))
    inputs = (by_expert(source), by_expert(pick_slot), by_expert(filled), by_expert(slot_weight),
              gate_blocks, up_blocks, down_blocks)
    (token_acc, route_acc), (gate_all, up_all, down_all) = lax.scan(one_expert, start, inputs)
    scaled = (mix_gate[None, :] * cotangent.astype(jnp.float32)).astype(jnp.bfloat16)
    dense_dx = jnp.dot(scaled, dense_weight.T, preferred_element_type=jnp.float32)
    token_grad = (token_acc + dense_dx).astype(jnp.bfloat16)
    dense_grad = jnp.dot(tokens.T, scaled, preferred_element_type=jnp.float32) / N_EP
    dense_out = jnp.dot(tokens, dense_weight, preferred_element_type=jnp.float32)
    mix_grad = jnp.sum(cotangent.astype(jnp.float32) * dense_out, axis=0) / N_EP
    gate_grad = gate_all.reshape(EXPERTS * GROUP, D, FFB)
    up_grad = up_all.reshape(EXPERTS * GROUP, D, FFB)
    down_grad = down_all.reshape(EXPERTS * GROUP, FFB, D)
    return token_grad, route_acc, gate_grad, up_grad, down_grad, dense_grad, mix_grad
```

```python
import jax
import jax.numpy as jnp
from jax import lax
from jax.sharding import PartitionSpec as P

FF = 2816
BF = jnp.bfloat16
F32 = jnp.float32


def spread(values, group_size):
    experts = values.shape[0]
    copies = jnp.broadcast_to(values[:, None], (experts, group_size) + values.shape[1:])
    return copies.reshape((experts * group_size,) + values.shape[1:])


def swap(values, axis):
    return lax.all_to_all(values, axis, split_axis=0, concat_axis=0, tiled=True)


def local(tokens, cotangent, routes, route_weights, w_gate, w_up, w_down, dense_weight, mix_gate):
    tp_count = lax.axis_size("tp")
    ep_count = lax.axis_size("ep")
    slice_width = w_gate.shape[2]
    group_size = FF // (slice_width * tp_count)
    experts = ep_count // group_size
    token_count, top_count = routes.shape
    width_part = tokens.shape[1]
    width = width_part * tp_count
    capacity = 5 * token_count * top_count // (4 * experts)
    slots = experts * capacity
    rows_here = ep_count * capacity

    expert_ids = jnp.arange(experts, dtype=jnp.int32)
    named = routes[:, :, None] == expert_ids[None, None, :]
    member = jnp.any(named, axis=1)
    token_ids = jnp.arange(token_count, dtype=jnp.int32)
    before = (token_ids[:, None] > token_ids[None, :]).astype(BF)
    rank = jnp.dot(before, member.astype(BF), preferred_element_type=F32)
    weight_of = jnp.sum(jnp.where(named, route_weights.astype(F32)[:, :, None], 0.0), axis=1)
    slot_ids = jnp.arange(capacity, dtype=jnp.int32).astype(F32)
    rank_t = jnp.where(member, rank, -1.0).T
    hit = rank_t[:, None, :] == slot_ids[None, :, None]
    dispatch = hit.astype(BF).reshape(slots, token_count)
    slot_weight = jnp.sum(jnp.where(hit, weight_of.T[:, None, :], 0.0), axis=2).astype(BF)

    def pick(values):
        taken = jnp.dot(dispatch, values, preferred_element_type=F32).astype(BF)
        return spread(taken.reshape(experts, capacity, values.shape[1]), group_size)

    weights_in = swap(spread(slot_weight, group_size)[:, None, :], "ep").reshape(rows_here)
    rows_part = swap(pick(tokens), "ep")
    grads_full = lax.all_gather(cotangent, "tp", axis=1, tiled=True)
    grads_in = swap(pick(grads_full), "ep").reshape(rows_here, width)
    rows_in = lax.all_gather(rows_part.reshape(rows_here, width_part), "tp", axis=1, tiled=True)

    dense_late, _ = lax.optimization_barrier((dense_weight, rows_part))
    dense_cols = dense_late.shape[1]
    gathered = swap(jnp.broadcast_to(dense_late[None], (ep_count,) + dense_late.shape), "ep")
    scaled = (mix_gate[None, :] * grads_full.astype(F32)).astype(BF)
    contract_rows = (((0,), (0,)), ((), ()))
    contract_cols = (((1,), (1,)), ((), ()))
    product = lax.dot_general(tokens, scaled, contract_rows, preferred_element_type=F32).astype(BF)
    product = product.reshape(width_part, ep_count, dense_cols).transpose(1, 0, 2)

    gate_matrix = w_gate[0]
    up_matrix = w_up[0]
    down_matrix = w_down[0]
    pre_gate = jnp.dot(rows_in, gate_matrix, preferred_element_type=F32)
    pre_up = jnp.dot(rows_in, up_matrix, preferred_element_type=F32)
    sigmoid_gate = jax.nn.sigmoid(pre_gate)
    activated = pre_gate * sigmoid_gate
    hidden = activated * pre_up
    hidden_bf = hidden.astype(BF)
    projected = lax.dot_general(grads_in, down_matrix, contract_cols, preferred_element_type=F32)
    route_part = jnp.sum(hidden_bf.astype(F32) * projected, axis=1)
    weight_col = weights_in.astype(F32)[:, None]
    hidden_grad = weight_col * projected
    d_gate = (hidden_grad * pre_up * sigmoid_gate * (1.0 + pre_gate * (1.0 - sigmoid_gate))).astype(BF)
    d_up = (hidden_grad * activated).astype(BF)
    weighted = (weight_col * hidden).astype(BF)
    partial_value = (
        lax.dot_general(d_gate, gate_matrix, contract_cols, preferred_element_type=F32)
        + lax.dot_general(d_up, up_matrix, contract_cols, preferred_element_type=F32)
    ).astype(BF)
    mixed = lax.all_to_all(partial_value, "tp", split_axis=1, concat_axis=0, tiled=True)
    column_sum = jnp.sum(mixed.reshape(tp_count, rows_here, -1).astype(F32), axis=0).astype(BF)
    returned = swap(column_sum.reshape(ep_count, capacity, width_part), "ep")

    product_late, _ = lax.optimization_barrier((product, grads_in))
    shares = swap(product_late, "ep")
    dense_grad = jnp.sum(shares.astype(F32), axis=0) * (1.0 / ep_count)

    moment = lax.dot_general(tokens, grads_full, contract_rows, preferred_element_type=F32)
    moment = moment.reshape(width_part, ep_count, dense_cols)
    gain = jnp.sum(gathered.astype(F32) * moment.transpose(1, 0, 2), axis=1).reshape(1, width)
    devices = ep_count * tp_count
    route_rows = jnp.broadcast_to(
        route_part.reshape(ep_count, 1, capacity), (ep_count, tp_count, capacity)
    ).reshape(devices, capacity)
    packed = jnp.concatenate([jnp.broadcast_to(gain, (devices, width)), route_rows], axis=1)
    small = swap(packed[:, None, :], ("ep", "tp")).reshape(devices, width + capacity)
    mix_grad = jnp.sum(small[:, :width], axis=0) * (1.0 / ep_count)
    slot_route = jnp.sum(
        small[:, width:].reshape(experts, group_size * tp_count, capacity), axis=1
    )
    expert_route = jnp.sum(jnp.where(hit, slot_route[:, :, None], 0.0), axis=1).T
    route_grad = jnp.sum(jnp.where(named, expert_route[:, None, :], 0.0), axis=2)

    gate_grad = lax.dot_general(rows_in, d_gate, contract_rows, preferred_element_type=F32)
    up_grad = lax.dot_general(rows_in, d_up, contract_rows, preferred_element_type=F32)
    down_grad = lax.dot_general(weighted, grads_in, contract_rows, preferred_element_type=F32)

    back = returned.reshape(experts, group_size, capacity, width_part)
    combine = jnp.broadcast_to(hit[:, None], (experts, group_size) + hit.shape[1:]).astype(BF)
    expert_grad = lax.dot_general(
        combine.reshape(rows_here, token_count),
        back.reshape(rows_here, width_part),
        contract_rows,
        preferred_element_type=F32,
    )
    whole_weight = gathered.transpose(1, 0, 2).reshape(width_part, width)
    dense_dx = lax.dot_general(scaled, whole_weight, contract_cols, preferred_element_type=F32)
    token_grad = (expert_grad + dense_dx).astype(BF)
    return (
        token_grad,
        route_grad,
        gate_grad.astype(BF)[None],
        up_grad.astype(BF)[None],
        down_grad.astype(BF)[None],
        dense_grad,
        mix_grad,
    )


def solution(mesh):
    return jax.shard_map(
        local,
        mesh=mesh,
        in_specs=(
            P("ep", "tp"),
            P("ep", "tp"),
            P("ep", None),
            P("ep", None),
            P("ep", None, "tp"),
            P("ep", None, "tp"),
            P("ep", "tp", None),
            P("tp", "ep"),
            P(),
        ),
        out_specs=(
            P("ep", "tp"),
            P("ep", None),
            P("ep", None, "tp"),
            P("ep", None, "tp"),
            P("ep", "tp", None),
            P("tp", "ep"),
            P(),
        ),
        check_vma=False,
    )
```

```python
import jax
import jax.numpy as jnp
from jax import lax
from jax.sharding import PartitionSpec as P

FF = 2816
BF = jnp.bfloat16
F32 = jnp.float32


def spread(values, group_size):
    experts = values.shape[0]
    copies = jnp.broadcast_to(values[:, None], (experts, group_size) + values.shape[1:])
    return copies.reshape((experts * group_size,) + values.shape[1:])


def swap(values, axis):
    return lax.all_to_all(values, axis, split_axis=0, concat_axis=0, tiled=True)


def local(tokens, cotangent, routes, route_weights, w_gate, w_up, w_down, dense_weight, mix_gate):
    tp_count = lax.axis_size("tp")
    ep_count = lax.axis_size("ep")
    slice_width = w_gate.shape[2]
    group_size = FF // (slice_width * tp_count)
    experts = ep_count // group_size
    token_count, top_count = routes.shape
    width_part = tokens.shape[1]
    width = width_part * tp_count
    capacity = 5 * token_count * top_count // (4 * experts)
    slots = experts * capacity
    rows_here = ep_count * capacity

    expert_ids = jnp.arange(experts, dtype=jnp.int32)
    named = routes[:, :, None] == expert_ids[None, None, :]
    member = jnp.any(named, axis=1)
    token_ids = jnp.arange(token_count, dtype=jnp.int32)
    before = (token_ids[:, None] > token_ids[None, :]).astype(BF)
    rank = jnp.dot(before, member.astype(BF), preferred_element_type=F32)
    weight_of = jnp.sum(jnp.where(named, route_weights.astype(F32)[:, :, None], 0.0), axis=1)
    slot_ids = jnp.arange(capacity, dtype=jnp.int32).astype(F32)
    rank_t = jnp.where(member, rank, -1.0).T
    hit = rank_t[:, None, :] == slot_ids[None, :, None]
    dispatch = hit.astype(BF).reshape(slots, token_count)
    slot_weight = jnp.sum(jnp.where(hit, weight_of.T[:, None, :], 0.0), axis=2).astype(BF)

    def pick(values):
        taken = jnp.dot(dispatch, values, preferred_element_type=F32).astype(BF)
        return spread(taken.reshape(experts, capacity, values.shape[1]), group_size)

    rows_part = swap(pick(tokens), "ep")
    grads_full = lax.all_gather(cotangent, "tp", axis=1, tiled=True)
    lanes = jnp.broadcast_to(spread(slot_weight, group_size)[:, :, None], (ep_count, capacity, 128))
    arrived = swap(jnp.concatenate([pick(grads_full), lanes], axis=2), "ep")
    arrived = arrived.reshape(rows_here, width + 128)
    grads_in, weight_col = arrived[:, :width], arrived[:, width : width + 1].astype(F32)
    rows_in = lax.all_gather(rows_part.reshape(rows_here, width_part), "tp", axis=1, tiled=True)

    contract_rows = (((0,), (0,)), ((), ()))
    contract_cols = (((1,), (1,)), ((), ()))
    dense_cols = dense_weight.shape[1]
    scaled = (mix_gate[None, :] * grads_full.astype(F32)).astype(BF)
    product = lax.dot_general(tokens, scaled, contract_rows, preferred_element_type=F32).astype(BF)
    product = product.reshape(width_part, ep_count, dense_cols).transpose(1, 0, 2)
    copies = jnp.broadcast_to(dense_weight[None], (ep_count,) + dense_weight.shape)
    outgoing, _ = lax.optimization_barrier((jnp.concatenate([copies, product], axis=1), arrived))
    met = swap(outgoing, "ep")
    gathered, shares = met[:, :width_part], met[:, width_part:]
    dense_grad = jnp.sum(shares.astype(F32), axis=0) * (1.0 / ep_count)

    gate_matrix = w_gate[0]
    up_matrix = w_up[0]
    down_matrix = w_down[0]
    pre_gate = jnp.dot(rows_in, gate_matrix, preferred_element_type=F32)
    pre_up = jnp.dot(rows_in, up_matrix, preferred_element_type=F32)
    sigmoid_gate = jax.nn.sigmoid(pre_gate)
    activated = pre_gate * sigmoid_gate
    hidden = activated * pre_up
    hidden_bf = hidden.astype(BF)
    projected = lax.dot_general(grads_in, down_matrix, contract_cols, preferred_element_type=F32)
    route_part = jnp.sum(hidden_bf.astype(F32) * projected, axis=1)
    hidden_grad = weight_col * projected
    d_gate = (hidden_grad * pre_up * sigmoid_gate * (1.0 + pre_gate * (1.0 - sigmoid_gate))).astype(BF)
    d_up = (hidden_grad * activated).astype(BF)
    weighted = (weight_col * hidden).astype(BF)
    partial_value = (
        lax.dot_general(d_gate, gate_matrix, contract_cols, preferred_element_type=F32)
        + lax.dot_general(d_up, up_matrix, contract_cols, preferred_element_type=F32)
    ).astype(BF)
    mixed = lax.all_to_all(partial_value, "tp", split_axis=1, concat_axis=0, tiled=True)
    column_sum = jnp.sum(mixed.reshape(tp_count, rows_here, -1).astype(F32), axis=0).astype(BF)
    returned = swap(column_sum.reshape(ep_count, capacity, width_part), "ep")

    moment = lax.dot_general(tokens, grads_full, contract_rows, preferred_element_type=F32)
    moment = moment.reshape(width_part, ep_count, dense_cols)
    gain = jnp.sum(gathered.astype(F32) * moment.transpose(1, 0, 2), axis=1).reshape(1, width)
    gain, route_part, _ = lax.optimization_barrier((gain, route_part, mixed))
    devices = ep_count * tp_count
    route_rows = jnp.broadcast_to(
        route_part.reshape(ep_count, 1, capacity), (ep_count, tp_count, capacity)
    ).reshape(devices, capacity)
    packed = jnp.concatenate([jnp.broadcast_to(gain, (devices, width)), route_rows], axis=1)
    small = swap(packed[:, None, :], ("ep", "tp")).reshape(devices, width + capacity)
    mix_grad = jnp.sum(small[:, :width], axis=0) * (1.0 / ep_count)
    slot_route = jnp.sum(
        small[:, width:].reshape(experts, group_size * tp_count, capacity), axis=1
    )
    expert_route = jnp.sum(jnp.where(hit, slot_route[:, :, None], 0.0), axis=1).T
    route_grad = jnp.sum(jnp.where(named, expert_route[:, None, :], 0.0), axis=2)

    gate_grad = lax.dot_general(rows_in, d_gate, contract_rows, preferred_element_type=F32)
    up_grad = lax.dot_general(rows_in, d_up, contract_rows, preferred_element_type=F32)
    down_grad = lax.dot_general(weighted, grads_in, contract_rows, preferred_element_type=F32)

    back = returned.reshape(experts, group_size, capacity, width_part)
    combine = jnp.broadcast_to(hit[:, None], (experts, group_size) + hit.shape[1:]).astype(BF)
    expert_grad = lax.dot_general(
        combine.reshape(rows_here, token_count),
        back.reshape(rows_here, width_part),
        contract_rows,
        preferred_element_type=F32,
    )
    whole_weight = gathered.transpose(1, 0, 2).reshape(width_part, width)
    dense_dx = lax.dot_general(scaled, whole_weight, contract_cols, preferred_element_type=F32)
    token_grad = (expert_grad + dense_dx).astype(BF)
    return (
        token_grad,
        route_grad,
        gate_grad.astype(BF)[None],
        up_grad.astype(BF)[None],
        down_grad.astype(BF)[None],
        dense_grad,
        mix_grad,
    )


def solution(mesh):
    return jax.shard_map(
        local,
        mesh=mesh,
        in_specs=(
            P("ep", "tp"),
            P("ep", "tp"),
            P("ep", None),
            P("ep", None),
            P("ep", None, "tp"),
            P("ep", None, "tp"),
            P("ep", "tp", None),
            P("tp", "ep"),
            P(),
        ),
        out_specs=(
            P("ep", "tp"),
            P("ep", None),
            P("ep", None, "tp"),
            P("ep", None, "tp"),
            P("ep", "tp", None),
            P("tp", "ep"),
            P(),
        ),
        check_vma=False,
    )
```
